32 devices in a mesh: sp: 16 (over z, y, x), dp: 2 (over core).
Axes of the slice: x: 2, y: 2, z: 4, core: 2. Of those that a mesh axis runs over, the one named last changes fastest.
Arguments:
- tokens: bfloat16 [4, 1024, 3072], P('dp', 'sp'), may hold values from -6 to 6
- pre_gain: float32 [3072], replicated, may hold values from 0.1 to 1.9
- in_weight: bfloat16 [3072, 1536], P('dp', 'sp'), may hold values from -0.109375 to 0.109375
- decay_rate: float32 [2, 96, 64], replicated, may hold values from 0 to 1, as said below
- frequency: float32 [2, 96, 64], replicated, may hold values from 1 to 200
- log_step: float32 [2, 96], replicated, may hold values from -3 to -2.3
- input_matrix: float32 [2, 2, 96, 1024], replicated, may hold values from -1 to 1
- output_matrix: float32 [2, 2, 96, 1024], replicated, may hold values from -0.5 to 0.5
- skip_gain: float32 [1536], replicated, may hold values from -4 to 4
- glu_weight: bfloat16 [1536, 1536], P('dp', 'sp'), may hold values from -0.15625 to 0.15625
- up_weight: bfloat16 [1536, 3072], P('dp', 'sp'), may hold values from -0.15625 to 0.15625
- post_gain: float32 [3072], replicated, may hold values from 0.1 to 1.9
Outputs:
- output: bfloat16 [4, 1024, 3072], P('dp', 'sp')
The draws below stay inside these ranges and needn't reach their ends.
Inputs may be any that keep to these rules, and one draw needn't show every extreme that they name: `decay_rate`: positive, for every direction, group and state.
All inputs are finite; a program needn't handle non-finite values.
Results may differ from the reference program's by a relative error of at most 0.0073.
Values may be sent and summed in bfloat16 or wider, within the bound.
A program may use at most 128 MiB of HBM per device.

```python
import jax
import jax.numpy as jnp
from jax import lax

D = 3072
WIDTH = 1536
GROUP = 16
STATE = 64
GROUPS = 96
SEQS = 4
LEN = 1024


def draw_decay_rate(key, part):
    key_kind, key_slow, key_fast = jax.random.split(key, 3)
    share = 0.5
    picked = jax.random.uniform(key_kind, (2, GROUPS, 1), jnp.float32)
    lower = jnp.log(4.0 / LEN)
    upper = jnp.log(20.0 / LEN)
    slow_rates = jnp.exp(jax.random.uniform(key_slow, (2, GROUPS, STATE), jnp.float32, lower, upper))
    fast_rates = jax.random.uniform(key_fast, (2, GROUPS, STATE), jnp.float32, 0.2, 0.6)
    return jnp.where(picked < share, slow_rates, fast_rates)


def block_levels(rng, shape, cuts, least, high):
    factor_of, own = 1.0, jax.random.fold_in(rng, 6)
    for position, parts in cuts:
        draws = jnp.exp(jax.random.uniform(jax.random.fold_in(own, position), (parts,), jnp.float32, least / len(cuts), high / len(cuts)))
        factor_of = factor_of * jnp.repeat(draws, shape[position] // parts).reshape([-1 if axis == position else 1 for axis in range(len(shape))])
    return factor_of


def normal_values(own_key, dims, deviation, reach, shards=(), kind=jnp.bfloat16):
    drawn = jax.random.normal(own_key, dims, jnp.float32) * deviation
    if len(shards) > 0:
        drawn = block_levels(own_key, dims, shards, -0.22, 0.18) * drawn
    return jnp.clip(drawn, min=-reach, max=reach).astype(kind)


def setup_inputs(seed: int = 0) -> dict:
    streams_of = jax.random.split(jax.random.key(seed), 13)
    tokens = normal_values(streams_of[0], (SEQS, LEN, D), 1.0, 6.0, ((0, 2), (1, 16)))
    pre_gain = jnp.clip(1.0 + 0.18 * jax.random.normal(streams_of[1], (D,), jnp.float32), 0.1, 1.9)
    in_weight = normal_values(streams_of[2], (D, WIDTH), D ** -0.5, 0.109375, ((0, 2), (1, 16)))
    decay_rate = draw_decay_rate(jax.random.fold_in(streams_of[12], 71), 0)
    frequency = jnp.clip(jax.random.uniform(streams_of[4], (2, GROUPS, STATE), jnp.float32, 1.0, 200.0), 1.0, 200.0)
    log_step = jnp.clip(jax.random.uniform(streams_of[5], (2, GROUPS), jnp.float32, -3.0, -2.3), -3.0, -2.3)
    input_matrix = normal_values(streams_of[6], (2, 2, GROUPS, STATE * GROUP), (2 * GROUP) ** -0.5, 1.0, (), jnp.float32)
    output_matrix = normal_values(streams_of[7], (2, 2, GROUPS, GROUP * STATE), (2 * STATE) ** -0.5, 0.5, (), jnp.float32)
    skip_gain = normal_values(streams_of[8], (WIDTH,), 1.0, 4.0, (), jnp.float32)
    glu_weight = normal_values(streams_of[9], (WIDTH, WIDTH), WIDTH ** -0.5, 0.15625, ((0, 2), (1, 16)))
    up_weight = normal_values(streams_of[10], (WIDTH, D), WIDTH ** -0.5, 0.15625, ((0, 2), (1, 16)))
    post_gain = jnp.clip(1.0 + 0.18 * jax.random.normal(streams_of[11], (D,), jnp.float32), 0.1, 1.9)
    return dict(tokens=tokens, pre_gain=pre_gain, in_weight=in_weight, decay_rate=decay_rate, frequency=frequency, log_step=log_step, input_matrix=input_matrix, output_matrix=output_matrix, skip_gain=skip_gain, glu_weight=glu_weight, up_weight=up_weight, post_gain=post_gain)


highest = lax.Precision.HIGHEST
epsilon = 1e-06

def rms_scale(values, gain):
    widened = values.astype(jnp.float32)
    return widened * lax.rsqrt(lax.optimization_barrier(jnp.mean(widened * widened, axis=-1, keepdims=True)) + epsilon) * gain

def complex_compose(earlier, later):
    return (later[0] * earlier[0] - later[1] * earlier[1], later[0] * earlier[1] + later[1] * earlier[0], later[0] * earlier[2] - later[1] * earlier[3] + later[2], later[0] * earlier[3] + later[1] * earlier[2] + later[3])

def discretize(decay_rate, frequency, log_step, input_matrix):
    groups, states = decay_rate.shape
    delta = jnp.exp(log_step)[:, None]
    damping = -decay_rate * delta
    turning = frequency * delta
    modulus = jnp.exp(damping)
    bar_re = modulus * jnp.cos(turning)
    bar_im = modulus * jnp.sin(turning)
    half_sine = jnp.sin(0.5 * turning)
    minus_re = jnp.expm1(damping) * jnp.cos(turning) - 2.0 * half_sine * half_sine
    denominator = decay_rate * decay_rate + frequency * frequency
    factor_re = (bar_im * frequency - minus_re * decay_rate) / denominator
    factor_im = (-bar_im * decay_rate - minus_re * frequency) / denominator
    matrix_re = input_matrix[0].reshape(groups, states, -1)
    matrix_im = input_matrix[1].reshape(groups, states, -1)
    bbar_re = factor_re[..., None] * matrix_re - factor_im[..., None] * matrix_im
    bbar_im = factor_re[..., None] * matrix_im + factor_im[..., None] * matrix_re
    return (bar_re, bar_im, bbar_re, bbar_im)

def scan_groups(inputs, bar_re, bar_im, bbar_re, bbar_im, out_re, out_im, reverse):
    drive_re = jnp.einsum('kph,khl->kpl', bbar_re, inputs, precision=highest)
    drive_im = jnp.einsum('kph,khl->kpl', bbar_im, inputs, precision=highest)
    extent = drive_re.shape
    decay_re = jnp.broadcast_to(bar_re[:, :, None], extent)
    decay_im = jnp.broadcast_to(bar_im[:, :, None], extent)
    scanned = lax.associative_scan(complex_compose, (decay_re, decay_im, drive_re, drive_im), reverse=reverse, axis=2)
    return jnp.einsum('khp,kpl->khl', out_re, scanned[2], precision=highest) - jnp.einsum('khp,kpl->khl', out_im, scanned[3], precision=highest)

def reference(tokens, pre_gain, in_weight, decay_rate, frequency, log_step, input_matrix, output_matrix, skip_gain, glu_weight, up_weight, post_gain):
    bundle = 8
    bundles = GROUPS // bundle

    def regroup(array):
        return array.reshape((bundles, bundle) + array.shape[1:])
    tables = ()
    for direction in range(2):
        bar_re, bar_im, bbar_re, bbar_im = discretize(decay_rate[direction], frequency[direction], log_step[direction], input_matrix[direction])
        out_re = output_matrix[direction, 0].reshape(GROUPS, GROUP, STATE)
        out_im = output_matrix[direction, 1].reshape(GROUPS, GROUP, STATE)
        tables = tables + tuple((regroup(table) for table in (bar_re, bar_im, bbar_re, bbar_im, out_re, out_im)))

    def one_sequence(sequence):
        normed = rms_scale(sequence, pre_gain).astype(jnp.bfloat16)
        mixer_in = jnp.dot(normed, in_weight, preferred_element_type=jnp.float32).astype(jnp.bfloat16)
        widened = mixer_in.astype(jnp.float32)
        grouped = jnp.transpose(widened.reshape(LEN, GROUPS, GROUP), (1, 2, 0))

        def one_batch(packed):
            inputs = packed[0]
            forward = scan_groups(inputs, *packed[1:7], False)
            backward = scan_groups(inputs, *packed[7:13], True)
            return forward + backward
        scanned = lax.map(one_batch, (regroup(grouped),) + tables)
        scanned = jnp.transpose(scanned.reshape(GROUPS * GROUP, LEN))
        mixed = jax.nn.gelu(scanned + skip_gain * widened).astype(jnp.bfloat16)
        gate_pre = jnp.dot(mixed, glu_weight, preferred_element_type=jnp.float32)
        gated = (mixed.astype(jnp.float32) * jax.nn.sigmoid(gate_pre)).astype(jnp.bfloat16)
        projected = jnp.dot(gated, up_weight, preferred_element_type=jnp.float32)
        return rms_scale(projected, post_gain).astype(jnp.bfloat16)
    return lax.map(one_sequence, tokens)
```

```python
import functools

import jax
import jax.numpy as jnp
from jax import lax
from jax.experimental import pallas as pl
from jax.experimental.pallas import tpu as pltpu
from jax.sharding import PartitionSpec as P

epsilon = 1e-06
BLOCK = 16


def rms_scale(values, gain):
    widened = values.astype(jnp.float32)
    return widened * lax.rsqrt(jnp.mean(widened * widened, axis=-1, keepdims=True) + epsilon) * gain


def own_tables(decay_rate, frequency, log_step, input_matrix, output_matrix, offset, own, hop_steps):
    take = functools.partial(lax.dynamic_slice_in_dim, start_index=offset, slice_size=own)
    rates = take(decay_rate, axis=1)
    frequencies = take(frequency, axis=1)
    delta = jnp.exp(take(log_step, axis=1))[..., None]
    damping = -rates * delta
    turning = frequencies * delta
    modulus = jnp.exp(damping)
    bar_im = modulus * jnp.sin(turning)
    half_sine = jnp.sin(0.5 * turning)
    minus_re = jnp.expm1(damping) * jnp.cos(turning) - 2.0 * half_sine * half_sine
    denominator = rates * rates + frequencies * frequencies
    factor_re = (bar_im * frequencies - minus_re * rates) / denominator
    factor_im = (-bar_im * rates - minus_re * frequencies) / denominator
    states = rates.shape[-1]
    matrix = take(input_matrix, axis=2).reshape(2, 2, own, states, -1)
    readout = take(output_matrix, axis=2).reshape(2, 2, own, -1, states)
    bbar_re = factor_re[..., None] * matrix[:, 0] - factor_im[..., None] * matrix[:, 1]
    bbar_im = factor_re[..., None] * matrix[:, 1] + factor_im[..., None] * matrix[:, 0]

    def lanes(value):
        return jnp.transpose(value, (1, 2, 0, 3)).reshape(own, value.shape[2], 2 * states)

    b_re = lanes(jnp.swapaxes(bbar_re, 2, 3))
    b_im = lanes(jnp.swapaxes(bbar_im, 2, 3))
    c_re = lanes(readout[:, 0])
    c_im = lanes(readout[:, 1])
    step = jnp.arange(BLOCK, dtype=jnp.float32)
    last = BLOCK - 1.0
    hops = BLOCK * 2.0 ** jnp.arange(hop_steps, dtype=jnp.float32)
    forward = jnp.concatenate([last - step, step + 1.0, step - last, hops])
    backward = jnp.concatenate([step, BLOCK - step, -step, hops])
    exponent = jnp.stack([forward, backward])[:, None, :, None]
    size = jnp.exp(damping[:, :, None, :] * exponent)
    angle = turning[:, :, None, :] * exponent
    return b_re, b_im, c_re, c_im, lanes(size * jnp.cos(angle)), lanes(size * jnp.sin(angle))


def table_kernel(b_re, b_im, c_re, c_im, p_re, p_im, within, enter, leave, inner_ref):
    channels, lanes = b_re.shape[1:]
    bre, bim, cre, cim = b_re[0], b_im[0], c_re[0], c_im[0]
    for step in range(BLOCK):
        rows = pl.ds(step * channels, channels)

        def power(which):
            row = which * BLOCK + step
            return p_re[0, row : row + 1, :], p_im[0, row : row + 1, :]

        wre, wim = power(0)
        enter[0, rows, :lanes] = (wre * bre - wim * bim).astype(jnp.bfloat16)
        enter[0, rows, lanes:] = (wre * bim + wim * bre).astype(jnp.bfloat16)
        vre, vim = power(1)
        leave[0, rows, :lanes] = (vre * cre - vim * cim).astype(jnp.bfloat16)
        leave[0, rows, lanes:] = (-vre * cim - vim * cre).astype(jnp.bfloat16)
        xre, xim = power(2)
        inner_ref[rows, :lanes] = (xre * cre - xim * cim).astype(jnp.bfloat16)
        inner_ref[rows, lanes:] = (-xre * cim - xim * cre).astype(jnp.bfloat16)
    side = enter[0].shape[0]
    lane = lax.broadcasted_iota(jnp.int32, (side, 2 * lanes), 1) % lanes
    entering = enter[0]
    contract = (((1,), (1,)), ((), ()))
    zero = jnp.zeros_like(entering)
    ahead = lax.dot_general(
        jnp.where(lane < lanes // 2, entering, zero), inner_ref[...], contract,
        preferred_element_type=jnp.float32,
    )
    behind = lax.dot_general(
        jnp.where(lane < lanes // 2, zero, entering), inner_ref[...], contract,
        preferred_element_type=jnp.float32,
    )
    source = lax.broadcasted_iota(jnp.int32, (side, side), 0) // channels
    target = lax.broadcasted_iota(jnp.int32, (side, side), 1) // channels
    within[0] = (
        jnp.where(source <= target, ahead, 0.0) + jnp.where(source >= target, behind, 0.0)
    ).astype(jnp.bfloat16)


def make_tables(tables):
    own, channels, lanes = tables[0].shape
    side = BLOCK * channels
    whole = lambda value: pl.BlockSpec((1,) + value.shape[1:], lambda g: (g, 0, 0))
    out = lambda width: jax.ShapeDtypeStruct((own, side, width), jnp.bfloat16)
    outs = (out(side), out(2 * lanes), out(2 * lanes))
    return pl.pallas_call(
        table_kernel,
        grid=(own,),
        out_shape=outs,
        in_specs=[whole(value) for value in tables],
        out_specs=[whole(value) for value in outs],
        scratch_shapes=[pltpu.VMEM((side, 2 * lanes), jnp.bfloat16)],
        cost_estimate=pl.CostEstimate(
            flops=own * 4 * side * side * 2 * lanes * 4, bytes_accessed=own * side * side * 6, transcendentals=0
        ),
        name="tables",
    )(*tables)


def scan_kernel(length, u_ref, within, enter, leave, p_re, p_im, skip, out_ref):
    lanes = p_re.shape[2]
    rows = u_ref.shape[1]
    u = u_ref[0]
    local = jnp.dot(u, enter[0], preferred_element_type=jnp.float32)
    s_re, s_im = local[:, :lanes], local[:, lanes:]
    lane = lax.broadcasted_iota(jnp.int32, (rows, lanes), 1)
    place = lax.broadcasted_iota(jnp.int32, (rows, lanes), 0) % length
    forward = lane < lanes // 2

    def shifted(value, by):
        pad = jnp.zeros((by, lanes), jnp.float32)
        down = jnp.concatenate([pad, value[:-by]], axis=0)
        up = jnp.concatenate([value[by:], pad], axis=0)
        down = jnp.where(place >= by, down, 0.0)
        up = jnp.where(place < length - by, up, 0.0)
        return jnp.where(forward, down, up)

    hop = 1
    row = 3 * BLOCK
    while hop < length:
        h_re, h_im = p_re[0, row : row + 1, :], p_im[0, row : row + 1, :]
        m_re, m_im = shifted(s_re, hop), shifted(s_im, hop)
        s_re, s_im = s_re + h_re * m_re - h_im * m_im, s_im + h_re * m_im + h_im * m_re
        hop, row = 2 * hop, row + 1
    held = jnp.concatenate([shifted(s_re, 1), shifted(s_im, 1)], axis=1).astype(jnp.bfloat16)
    total = jnp.dot(u, within[0], preferred_element_type=jnp.float32)
    total += lax.dot_general(
        held, leave[0], (((1,), (1,)), ((), ())), preferred_element_type=jnp.float32
    )
    out_ref[0] = jax.nn.gelu(total + skip[0] * u.astype(jnp.float32)).astype(jnp.bfloat16)


def run_scan(blocks, within, enter, leave, p_re, p_im, skip, length):
    own, rows, side = blocks.shape
    whole = lambda value: pl.BlockSpec((1,) + value.shape[1:], lambda g: (g, 0, 0))
    operands = (blocks, within, enter, leave, p_re, p_im, skip)
    return pl.pallas_call(
        functools.partial(scan_kernel, length),
        grid=(own,),
        out_shape=jax.ShapeDtypeStruct(blocks.shape, jnp.bfloat16),
        in_specs=[whole(value) for value in operands],
        out_specs=whole(blocks),
        name="mixer",
    )(*operands)


def per_device(
    tokens,
    pre_gain,
    in_weight,
    decay_rate,
    frequency,
    log_step,
    input_matrix,
    output_matrix,
    skip_gain,
    glu_weight,
    up_weight,
    post_gain,
):
    def gather(weight):
        columns = lax.all_gather(weight, "sp", axis=1, tiled=True)
        return lax.all_gather(columns, "dp", axis=0, tiled=True)

    seqs, local_len, _ = tokens.shape
    sp = lax.axis_size("sp")
    group_size = input_matrix.shape[-1] // decay_rate.shape[2]
    groups = decay_rate.shape[1]
    own = groups // sp
    near = local_len // BLOCK
    side = BLOCK * group_size
    length = near * sp
    offset = lax.axis_index("sp") * own

    in_full = gather(in_weight)
    tables = own_tables(
        decay_rate, frequency, log_step, input_matrix, output_matrix, offset, own,
        max(1, (length - 1).bit_length()),
    )
    within, enter, leave = make_tables(tables)
    skip_rows = lax.dynamic_slice_in_dim(skip_gain.reshape(groups, 1, group_size), offset, own, 0)
    skip_rows = jnp.tile(skip_rows, (1, 1, BLOCK))
    normed = rms_scale(tokens, pre_gain).astype(jnp.bfloat16)
    mixer_in = jnp.einsum(
        "std,dw->stw", normed, in_full, preferred_element_type=jnp.float32
    ).astype(jnp.bfloat16)
    glu_full, up_full = gather(glu_weight), gather(up_weight)
    blocks = mixer_in.reshape(seqs, near, BLOCK, groups, group_size)
    blocks = jnp.transpose(blocks, (3, 0, 1, 2, 4)).reshape(groups, seqs, near, side)
    blocks = lax.all_to_all(blocks, "sp", split_axis=0, concat_axis=2, tiled=True)
    mixed = run_scan(
        blocks.reshape(own, seqs * length, side), within, enter, leave, tables[4], tables[5],
        skip_rows, length,
    )
    mixed = mixed.reshape(own, seqs, length, side)
    mixed = lax.all_to_all(mixed, "sp", split_axis=2, concat_axis=0, tiled=True)
    mixed = mixed.reshape(groups, seqs, near, BLOCK, group_size)
    mixed = jnp.transpose(mixed, (1, 2, 3, 0, 4)).reshape(seqs, local_len, groups * group_size)
    gate_pre = jnp.einsum("stw,wv->stv", mixed, glu_full, preferred_element_type=jnp.float32)
    gated = (mixed.astype(jnp.float32) * jax.nn.sigmoid(gate_pre)).astype(jnp.bfloat16)
    projected = jnp.einsum("stw,wd->std", gated, up_full, preferred_element_type=jnp.float32)
    return rms_scale(projected, post_gain).astype(jnp.bfloat16)


def solution(mesh):
    return jax.shard_map(
        per_device,
        mesh=mesh,
        in_specs=(
            P("dp", "sp", None),
            P(),
            P("dp", "sp"),
            P(),
            P(),
            P(),
            P(),
            P(),
            P(),
            P("dp", "sp"),
            P("dp", "sp"),
            P(),
        ),
        out_specs=P("dp", "sp", None),
        check_vma=False,
    )
```

```python
import functools

import jax
import jax.numpy as jnp
from jax import lax
from jax.experimental import pallas as pl
from jax.experimental.pallas import tpu as pltpu
from jax.sharding import PartitionSpec as P

epsilon = 1e-06
BLOCK = 16


def rms_scale(values, gain):
    widened = values.astype(jnp.float32)
    return widened * lax.rsqrt(jnp.mean(widened * widened, axis=-1, keepdims=True) + epsilon) * gain


def own_tables(decay_rate, frequency, log_step, input_matrix, output_matrix, offset, own, hop_steps):
    take = functools.partial(lax.dynamic_slice_in_dim, start_index=offset, slice_size=own)
    rates = take(decay_rate, axis=1)
    frequencies = take(frequency, axis=1)
    delta = jnp.exp(take(log_step, axis=1))[..., None]
    damping = -rates * delta
    turning = frequencies * delta
    modulus = jnp.exp(damping)
    bar_im = modulus * jnp.sin(turning)
    half_sine = jnp.sin(0.5 * turning)
    minus_re = jnp.expm1(damping) * jnp.cos(turning) - 2.0 * half_sine * half_sine
    denominator = rates * rates + frequencies * frequencies
    factor_re = (bar_im * frequencies - minus_re * rates) / denominator
    factor_im = (-bar_im * rates - minus_re * frequencies) / denominator
    states = rates.shape[-1]
    matrix = take(input_matrix, axis=2).reshape(2, 2, own, states, -1)
    readout = take(output_matrix, axis=2).reshape(2, 2, own, -1, states)
    bbar_re = factor_re[..., None] * matrix[:, 0] - factor_im[..., None] * matrix[:, 1]
    bbar_im = factor_re[..., None] * matrix[:, 1] + factor_im[..., None] * matrix[:, 0]

    def lanes(value):
        return jnp.transpose(value, (1, 2, 0, 3)).reshape(own, value.shape[2], 2 * states)

    b_re = lanes(jnp.swapaxes(bbar_re, 2, 3))
    b_im = lanes(jnp.swapaxes(bbar_im, 2, 3))
    c_re = lanes(readout[:, 0])
    c_im = lanes(readout[:, 1])
    step = jnp.arange(BLOCK, dtype=jnp.float32)
    last = BLOCK - 1.0
    hops = BLOCK * 2.0 ** jnp.arange(hop_steps, dtype=jnp.float32)
    forward = jnp.concatenate([last - step, step + 1.0, step - last, hops])
    backward = jnp.concatenate([step, BLOCK - step, -step, hops])
    exponent = jnp.stack([forward, backward])[:, None, :, None]
    size = jnp.exp(damping[:, :, None, :] * exponent)
    angle = turning[:, :, None, :] * exponent
    return b_re, b_im, c_re, c_im, lanes(size * jnp.cos(angle)), lanes(size * jnp.sin(angle))


MESH = pl.DeviceIdType.MESH


def gather_kernel(sp, dp, shard, out, own_sem, send_sem, recv_sem, pass_sem, take_sem):
    rows, depth = shard.shape
    n_y, n_x = 2, 2
    n_z = sp // (n_y * n_x)
    me, core = lax.axis_index("sp"), lax.axis_index("dp")
    z, y, x = me // (n_y * n_x), (me // n_x) % n_y, me % n_x
    first = (rows // 2 + 15) // 16 * 16
    halves = ((0, first), (first, rows - first))

    def index(z_at, y_at, x_at):
        return (z_at * n_y + y_at) * n_x + x_at

    y_other, x_other = (y + 1) % n_y, (x + 1) % n_x
    y_peer, x_peer = index(z, y_other, x), index(z, y, x_other)
    z_peers = [index((z + hop) % n_z, y, x) for hop in range(1, n_z)]
    cores = [(core + hop) % dp for hop in range(1, dp)]
    barrier = pltpu.get_barrier_semaphore()
    for peer in [y_peer, x_peer] + z_peers:
        pl.semaphore_signal(barrier, inc=1, device_id={"sp": peer}, device_id_type=MESH)
    for peer in cores:
        pl.semaphore_signal(barrier, inc=1, device_id={"dp": peer}, device_id_type=MESH)
    pl.semaphore_wait(barrier, 2 + len(z_peers) + len(cores))

    sent, passed = [], []

    def place(who, half, column):
        start, size = halves[half]
        return out.at[
            pl.ds(pl.multiple_of(who * rows + start, 16), size),
            pl.ds(pl.multiple_of(column * depth, 128), depth),
        ]

    def source(who, half, mine):
        return shard.at[pl.ds(*halves[half]), :] if mine else place(who, half, core)

    def send(who, half, peer, mine=False):
        copy = pltpu.make_async_remote_copy(
            src_ref=source(who, half, mine),
            dst_ref=place(who, half, core),
            send_sem=send_sem.at[len(sent)],
            recv_sem=recv_sem.at[who, half],
            device_id={"sp": peer},
            device_id_type=MESH,
        )
        copy.start()
        sent.append(copy)

    def spread(who, half, mine=False):
        for hop, peer in enumerate(cores):
            copy = pltpu.make_async_remote_copy(
                src_ref=source(who, half, mine),
                dst_ref=place(who, half, core),
                send_sem=pass_sem.at[len(passed)],
                recv_sem=take_sem.at[hop, who, half],
                device_id={"dp": peer},
                device_id_type=MESH,
            )
            copy.start()
            passed.append(copy)

    def arrived(who, half):
        pltpu.make_async_remote_copy(
            src_ref=place(who, half, core),
            dst_ref=place(who, half, core),
            send_sem=send_sem.at[0],
            recv_sem=recv_sem.at[who, half],
            device_id={"sp": y_peer},
            device_id_type=MESH,
        ).wait_recv()

    own = [
        pltpu.make_async_copy(source(me, half, True), place(me, half, core), own_sem.at[half])
        for half in range(2)
    ]
    send(me, 0, y_peer, True)
    send(me, 1, x_peer, True)
    for peer in z_peers:
        send(me, 0, peer, True)
        send(me, 1, peer, True)
    send(me, 0, x_peer, True)
    send(me, 1, y_peer, True)
    for half in range(2):
        own[half].start()
        spread(me, half, True)
    for hop in range(n_z):
        at = (z + n_z - hop) % n_z
        if hop > 0:
            here = index(at, y, x)
            arrived(here, 0)
            send(here, 0, y_peer)
            arrived(here, 1)
            send(here, 1, x_peer)
            send(here, 0, x_peer)
            send(here, 1, y_peer)
            spread(here, 0)
            spread(here, 1)
        by_y, by_x = index(at, y_other, x), index(at, y, x_other)
        arrived(by_y, 0)
        send(by_y, 0, x_peer)
        spread(by_y, 0)
        arrived(by_x, 1)
        send(by_x, 1, y_peer)
        spread(by_x, 1)
    for hop in range(n_z):
        at = (z + n_z - hop) % n_z
        by_y, by_x = index(at, y_other, x), index(at, y, x_other)
        across = index(at, y_other, x_other)
        for who, half in ((by_x, 0), (by_y, 1), (across, 0), (across, 1)):
            arrived(who, half)
            spread(who, half)
    for hop in range(1, dp):
        column = (core + dp - hop) % dp
        for who in range(sp):
            for half in range(2):
                pltpu.make_async_remote_copy(
                    src_ref=place(who, half, column),
                    dst_ref=place(who, half, column),
                    send_sem=pass_sem.at[0],
                    recv_sem=take_sem.at[hop - 1, who, half],
                    device_id={"dp": cores[0]},
                    device_id_type=MESH,
                ).wait_recv()
    for copy in own:
        copy.wait()
    for copy in sent + passed:
        copy.wait_send()


def relay_gather(shard, sp, dp):
    rows, depth = shard.shape
    return pl.pallas_call(
        functools.partial(gather_kernel, sp, dp),
        out_shape=jax.ShapeDtypeStruct((sp * rows, dp * depth), shard.dtype),
        in_specs=[pl.BlockSpec(memory_space=pltpu.VMEM)],
        out_specs=pl.BlockSpec(memory_space=pl.ANY),
        scratch_shapes=[
            pltpu.SemaphoreType.DMA((2,)),
            pltpu.SemaphoreType.DMA((8 * sp,)),
            pltpu.SemaphoreType.DMA((sp, 2)),
            pltpu.SemaphoreType.DMA((2 * sp * (dp - 1),)),
            pltpu.SemaphoreType.DMA((dp - 1, sp, 2)),
        ],
        compiler_params=pltpu.CompilerParams(collective_id=1, has_side_effects=True),
        cost_estimate=pl.CostEstimate(flops=10**8, bytes_accessed=sp * rows * dp * depth * 2, transcendentals=0),
        name="relay_gather",
    )(shard)


def table_kernel(b_re, b_im, c_re, c_im, p_re, p_im, within, enter, leave, inner_ref):
    channels, lanes = b_re.shape[1:]
    bre, bim, cre, cim = b_re[0], b_im[0], c_re[0], c_im[0]
    for step in range(BLOCK):
        rows = pl.ds(step * channels, channels)

        def power(which):
            row = which * BLOCK + step
            return p_re[0, row : row + 1, :], p_im[0, row : row + 1, :]

        wre, wim = power(0)
        enter[0, rows, :lanes] = (wre * bre - wim * bim).astype(jnp.bfloat16)
        enter[0, rows, lanes:] = (wre * bim + wim * bre).astype(jnp.bfloat16)
        vre, vim = power(1)
        leave[0, rows, :lanes] = (vre * cre - vim * cim).astype(jnp.bfloat16)
        leave[0, rows, lanes:] = (-vre * cim - vim * cre).astype(jnp.bfloat16)
        xre, xim = power(2)
        inner_ref[rows, :lanes] = (xre * cre - xim * cim).astype(jnp.bfloat16)
        inner_ref[rows, lanes:] = (-xre * cim - xim * cre).astype(jnp.bfloat16)
    side = enter[0].shape[0]
    lane = lax.broadcasted_iota(jnp.int32, (side, 2 * lanes), 1) % lanes
    entering = enter[0]
    contract = (((1,), (1,)), ((), ()))
    zero = jnp.zeros_like(entering)
    ahead = lax.dot_general(
        jnp.where(lane < lanes // 2, entering, zero), inner_ref[...], contract,
        preferred_element_type=jnp.float32,
    )
    behind = lax.dot_general(
        jnp.where(lane < lanes // 2, zero, entering), inner_ref[...], contract,
        preferred_element_type=jnp.float32,
    )
    source = lax.broadcasted_iota(jnp.int32, (side, side), 0) // channels
    target = lax.broadcasted_iota(jnp.int32, (side, side), 1) // channels
    within[0] = (
        jnp.where(source <= target, ahead, 0.0) + jnp.where(source >= target, behind, 0.0)
    ).astype(jnp.bfloat16)


def make_tables(tables):
    own, channels, lanes = tables[0].shape
    side = BLOCK * channels
    whole = lambda value: pl.BlockSpec((1,) + value.shape[1:], lambda g: (g, 0, 0))
    out = lambda width: jax.ShapeDtypeStruct((own, side, width), jnp.bfloat16)
    outs = (out(side), out(2 * lanes), out(2 * lanes))
    return pl.pallas_call(
        table_kernel,
        grid=(own,),
        out_shape=outs,
        in_specs=[whole(value) for value in tables],
        out_specs=[whole(value) for value in outs],
        scratch_shapes=[pltpu.VMEM((side, 2 * lanes), jnp.bfloat16)],
        cost_estimate=pl.CostEstimate(
            flops=own * 4 * side * side * 2 * lanes * 4, bytes_accessed=own * side * side * 6, transcendentals=0
        ),
        name="tables",
    )(*tables)


def scan_kernel(length, u_ref, within, enter, leave, p_re, p_im, skip, out_ref):
    lanes = p_re.shape[2]
    rows = u_ref.shape[1]
    u = u_ref[0]
    local = jnp.dot(u, enter[0], preferred_element_type=jnp.float32)
    s_re, s_im = local[:, :lanes], local[:, lanes:]
    lane = lax.broadcasted_iota(jnp.int32, (rows, lanes), 1)
    place = lax.broadcasted_iota(jnp.int32, (rows, lanes), 0) % length
    forward = lane < lanes // 2

    def shifted(value, by):
        pad = jnp.zeros((by, lanes), jnp.float32)
        down = jnp.concatenate([pad, value[:-by]], axis=0)
        up = jnp.concatenate([value[by:], pad], axis=0)
        down = jnp.where(place >= by, down, 0.0)
        up = jnp.where(place < length - by, up, 0.0)
        return jnp.where(forward, down, up)

    hop = 1
    row = 3 * BLOCK
    while hop < length:
        h_re, h_im = p_re[0, row : row + 1, :], p_im[0, row : row + 1, :]
        m_re, m_im = shifted(s_re, hop), shifted(s_im, hop)
        s_re, s_im = s_re + h_re * m_re - h_im * m_im, s_im + h_re * m_im + h_im * m_re
        hop, row = 2 * hop, row + 1
    held = jnp.concatenate([shifted(s_re, 1), shifted(s_im, 1)], axis=1).astype(jnp.bfloat16)
    total = jnp.dot(u, within[0], preferred_element_type=jnp.float32)
    total += lax.dot_general(
        held, leave[0], (((1,), (1,)), ((), ())), preferred_element_type=jnp.float32
    )
    out_ref[0] = jax.nn.gelu(total + skip[0] * u.astype(jnp.float32)).astype(jnp.bfloat16)


def run_scan(blocks, within, enter, leave, p_re, p_im, skip, length):
    own, rows, side = blocks.shape
    whole = lambda value: pl.BlockSpec((1,) + value.shape[1:], lambda g: (g, 0, 0))
    operands = (blocks, within, enter, leave, p_re, p_im, skip)
    return pl.pallas_call(
        functools.partial(scan_kernel, length),
        grid=(own,),
        out_shape=jax.ShapeDtypeStruct(blocks.shape, jnp.bfloat16),
        in_specs=[whole(value) for value in operands],
        out_specs=whole(blocks),
        name="mixer",
    )(*operands)


def per_device(
    tokens,
    pre_gain,
    in_weight,
    decay_rate,
    frequency,
    log_step,
    input_matrix,
    output_matrix,
    skip_gain,
    glu_weight,
    up_weight,
    post_gain,
):
    seqs, local_len, _ = tokens.shape
    sp = lax.axis_size("sp")
    group_size = input_matrix.shape[-1] // decay_rate.shape[2]
    groups = decay_rate.shape[1]
    own = groups // sp
    near = local_len // BLOCK
    side = BLOCK * group_size
    length = near * sp
    offset = lax.axis_index("sp") * own

    dp = lax.axis_size("dp")
    packed = jnp.concatenate([glu_weight.T, up_weight.T], axis=0)
    glu_rows, packed_rows = glu_weight.shape[1], packed.shape[0]
    depth = packed.shape[1]
    packed = lax.all_gather(packed, "sp", axis=0, tiled=True)
    packed = lax.all_gather(packed, "dp", axis=0, tiled=True)
    packed = packed.reshape(dp, sp, packed_rows, depth)
    glu_full = packed[:, :, :glu_rows].reshape(dp, -1, depth)
    up_full = packed[:, :, glu_rows:].reshape(dp, -1, depth)
    in_full = relay_gather(in_weight.T, sp, dp)
    tables = own_tables(
        decay_rate, frequency, log_step, input_matrix, output_matrix, offset, own,
        max(1, (length - 1).bit_length()),
    )
    within, enter, leave = make_tables(tables)
    skip_rows = lax.dynamic_slice_in_dim(skip_gain.reshape(groups, 1, group_size), offset, own, 0)
    skip_rows = jnp.tile(skip_rows, (1, 1, BLOCK))
    normed = rms_scale(tokens, pre_gain).astype(jnp.bfloat16)
    mixer_in = jnp.einsum(
        "std,wd->stw", normed, in_full, preferred_element_type=jnp.float32
    ).astype(jnp.bfloat16)
    blocks = mixer_in.reshape(seqs, near, BLOCK, groups, group_size)
    blocks = jnp.transpose(blocks, (3, 0, 1, 2, 4)).reshape(groups, seqs, near, side)
    blocks = lax.all_to_all(blocks, "sp", split_axis=0, concat_axis=2, tiled=True)
    mixed = run_scan(
        blocks.reshape(own, seqs * length, side), within, enter, leave, tables[4], tables[5],
        skip_rows, length,
    )
    mixed = mixed.reshape(own, seqs, length, side)
    mixed = lax.all_to_all(mixed, "sp", split_axis=2, concat_axis=0, tiled=True)
    mixed = mixed.reshape(groups, seqs, near, BLOCK, group_size)
    mixed = jnp.transpose(mixed, (1, 2, 3, 0, 4)).reshape(seqs, local_len, groups * group_size)
    def project(rows, weight):
        parts = [
            jnp.einsum(
                "stw,vw->stv", rows[..., k * depth : (k + 1) * depth], weight[k],
                preferred_element_type=jnp.float32,
            )
            for k in range(dp)
        ]
        return functools.reduce(jnp.add, parts)

    gate_pre = project(mixed, glu_full)
    gated = (mixed.astype(jnp.float32) * jax.nn.sigmoid(gate_pre)).astype(jnp.bfloat16)
    projected = project(gated, up_full)
    return rms_scale(projected, post_gain).astype(jnp.bfloat16)


def solution(mesh):
    return jax.shard_map(
        per_device,
        mesh=mesh,
        in_specs=(
            P("dp", "sp", None),
            P(),
            P("dp", "sp"),
            P(),
            P(),
            P(),
            P(),
            P(),
            P(),
            P("dp", "sp"),
            P("dp", "sp"),
            P(),
        ),
        out_specs=P("dp", "sp", None),
        check_vma=False,
    )
```

```python
import functools

import jax
import jax.numpy as jnp
from jax import lax
from jax.experimental import pallas as pl
from jax.experimental.pallas import tpu as pltpu
from jax.sharding import PartitionSpec as P


epsilon = 1e-06
BLOCK = 16


def rms_scale(values, gain):
    widened = values.astype(jnp.float32)
    return widened * lax.rsqrt(jnp.mean(widened * widened, axis=-1, keepdims=True) + epsilon) * gain


def own_tables(decay_rate, frequency, log_step, input_matrix, output_matrix, offset, own, hop_steps):
    take = functools.partial(lax.dynamic_slice_in_dim, start_index=offset, slice_size=own)
    rates = take(decay_rate, axis=1)
    frequencies = take(frequency, axis=1)
    delta = jnp.exp(take(log_step, axis=1))[..., None]
    damping = -rates * delta
    turning = frequencies * delta
    modulus = jnp.exp(damping)
    bar_im = modulus * jnp.sin(turning)
    half_sine = jnp.sin(0.5 * turning)
    minus_re = jnp.expm1(damping) * jnp.cos(turning) - 2.0 * half_sine * half_sine
    denominator = rates * rates + frequencies * frequencies
    factor_re = (bar_im * frequencies - minus_re * rates) / denominator
    factor_im = (-bar_im * rates - minus_re * frequencies) / denominator
    states = rates.shape[-1]
    matrix = take(input_matrix, axis=2).reshape(2, 2, own, states, -1)
    readout = take(output_matrix, axis=2).reshape(2, 2, own, -1, states)
    bbar_re = factor_re[..., None] * matrix[:, 0] - factor_im[..., None] * matrix[:, 1]
    bbar_im = factor_re[..., None] * matrix[:, 1] + factor_im[..., None] * matrix[:, 0]

    def lanes(value):
        return jnp.transpose(value, (1, 2, 0, 3)).reshape(own, value.shape[2], 2 * states)

    b_re = lanes(jnp.swapaxes(bbar_re, 2, 3))
    b_im = lanes(jnp.swapaxes(bbar_im, 2, 3))
    c_re = lanes(readout[:, 0])
    c_im = lanes(readout[:, 1])
    step = jnp.arange(BLOCK, dtype=jnp.float32)
    last = BLOCK - 1.0
    hops = BLOCK * 2.0 ** jnp.arange(hop_steps, dtype=jnp.float32)
    forward = jnp.concatenate([last - step, step + 1.0, step - last, hops])
    backward = jnp.concatenate([step, BLOCK - step, -step, hops])
    exponent = jnp.stack([forward, backward])[:, None, :, None]
    size = jnp.exp(damping[:, :, None, :] * exponent)
    angle = turning[:, :, None, :] * exponent
    return b_re, b_im, c_re, c_im, lanes(size * jnp.cos(angle)), lanes(size * jnp.sin(angle))


MESH = pl.DeviceIdType.MESH


def gather_kernel(sp, dp, shard, out, own_sem, send_sem, recv_sem, pass_sem, take_sem):
    rows, depth = shard.shape
    n_y, n_x = 2, 2
    n_z = sp // (n_y * n_x)
    me, core = lax.axis_index("sp"), lax.axis_index("dp")
    z, y, x = me // (n_y * n_x), (me // n_x) % n_y, me % n_x
    first = (rows // 2 + 15) // 16 * 16
    halves = ((0, first), (first, rows - first))

    def index(z_at, y_at, x_at):
        return (z_at * n_y + y_at) * n_x + x_at

    y_other, x_other = (y + 1) % n_y, (x + 1) % n_x
    y_peer, x_peer = index(z, y_other, x), index(z, y, x_other)
    z_peers = [index((z + hop) % n_z, y, x) for hop in range(1, n_z)]
    cores = [(core + hop) % dp for hop in range(1, dp)]
    barrier = pltpu.get_barrier_semaphore()
    for peer in [y_peer, x_peer] + z_peers:
        pl.semaphore_signal(barrier, inc=1, device_id={"sp": peer}, device_id_type=MESH)
    for peer in cores:
        pl.semaphore_signal(barrier, inc=1, device_id={"dp": peer}, device_id_type=MESH)
    pl.semaphore_wait(barrier, 2 + len(z_peers) + len(cores))

    sent, passed = [], []

    def place(who, half, column):
        start, size = halves[half]
        return out.at[
            pl.ds(pl.multiple_of(who * rows + start, 16), size),
            pl.ds(pl.multiple_of(column * depth, 128), depth),
        ]

    def source(who, half, mine):
        return shard.at[pl.ds(*halves[half]), :] if mine else place(who, half, core)

    def send(who, half, peer, mine=False):
        copy = pltpu.make_async_remote_copy(
            src_ref=source(who, half, mine),
            dst_ref=place(who, half, core),
            send_sem=send_sem.at[len(sent)],
            recv_sem=recv_sem.at[who, half],
            device_id={"sp": peer},
            device_id_type=MESH,
        )
        copy.start()
        sent.append(copy)

    def spread(who, half, mine=False):
        for hop, peer in enumerate(cores):
            copy = pltpu.make_async_remote_copy(
                src_ref=source(who, half, mine),
                dst_ref=place(who, half, core),
                send_sem=pass_sem.at[len(passed)],
                recv_sem=take_sem.at[hop, who, half],
                device_id={"dp": peer},
                device_id_type=MESH,
            )
            copy.start()
            passed.append(copy)

    def arrived(who, half):
        pltpu.make_async_remote_copy(
            src_ref=place(who, half, core),
            dst_ref=place(who, half, core),
            send_sem=send_sem.at[0],
            recv_sem=recv_sem.at[who, half],
            device_id={"sp": y_peer},
            device_id_type=MESH,
        ).wait_recv()

    own = [
        pltpu.make_async_copy(source(me, half, True), place(me, half, core), own_sem.at[half])
        for half in range(2)
    ]
    send(me, 0, y_peer, True)
    send(me, 1, x_peer, True)
    for peer in z_peers:
        send(me, 0, peer, True)
        send(me, 1, peer, True)
    send(me, 0, x_peer, True)
    send(me, 1, y_peer, True)
    for half in range(2):
        own[half].start()
        spread(me, half, True)
    for hop in range(n_z):
        at = (z + n_z - hop) % n_z
        if hop > 0:
            here = index(at, y, x)
            arrived(here, 0)
            send(here, 0, y_peer)
            arrived(here, 1)
            send(here, 1, x_peer)
            send(here, 0, x_peer)
            send(here, 1, y_peer)
            spread(here, 0)
            spread(here, 1)
        by_y, by_x = index(at, y_other, x), index(at, y, x_other)
        arrived(by_y, 0)
        send(by_y, 0, x_peer)
        spread(by_y, 0)
        arrived(by_x, 1)
        send(by_x, 1, y_peer)
        spread(by_x, 1)
    for hop in range(n_z):
        at = (z + n_z - hop) % n_z
        by_y, by_x = index(at, y_other, x), index(at, y, x_other)
        across = index(at, y_other, x_other)
        for who, half in ((by_x, 0), (by_y, 1), (across, 0), (across, 1)):
            arrived(who, half)
            spread(who, half)
    for hop in range(1, dp):
        column = (core + dp - hop) % dp
        for who in range(sp):
            for half in range(2):
                pltpu.make_async_remote_copy(
                    src_ref=place(who, half, column),
                    dst_ref=place(who, half, column),
                    send_sem=pass_sem.at[0],
                    recv_sem=take_sem.at[hop - 1, who, half],
                    device_id={"dp": cores[0]},
                    device_id_type=MESH,
                ).wait_recv()
    for copy in own:
        copy.wait()
    for copy in sent + passed:
        copy.wait_send()


def relay_gather(shard, sp, dp):
    rows, depth = shard.shape
    return pl.pallas_call(
        functools.partial(gather_kernel, sp, dp),
        out_shape=jax.ShapeDtypeStruct((sp * rows, dp * depth), shard.dtype),
        in_specs=[pl.BlockSpec(memory_space=pltpu.VMEM)],
        out_specs=pl.BlockSpec(memory_space=pl.ANY),
        scratch_shapes=[
            pltpu.SemaphoreType.DMA((2,)),
            pltpu.SemaphoreType.DMA((8 * sp,)),
            pltpu.SemaphoreType.DMA((sp, 2)),
            pltpu.SemaphoreType.DMA((2 * sp * (dp - 1),)),
            pltpu.SemaphoreType.DMA((dp - 1, sp, 2)),
        ],
        compiler_params=pltpu.CompilerParams(collective_id=1, has_side_effects=True),
        cost_estimate=pl.CostEstimate(flops=10**8, bytes_accessed=sp * rows * dp * depth * 2, transcendentals=0),
        name="relay_gather",
    )(shard)


def table_kernel(b_re, b_im, c_re, c_im, p_re, p_im, within, enter, leave, inner_ref):
    channels, lanes = b_re.shape[1:]
    bre, bim, cre, cim = b_re[0], b_im[0], c_re[0], c_im[0]
    for step in range(BLOCK):
        rows = pl.ds(step * channels, channels)

        def power(which):
            row = which * BLOCK + step
            return p_re[0, row : row + 1, :], p_im[0, row : row + 1, :]

        wre, wim = power(0)
        enter[0, rows, :lanes] = (wre * bre - wim * bim).astype(jnp.bfloat16)
        enter[0, rows, lanes:] = (wre * bim + wim * bre).astype(jnp.bfloat16)
        vre, vim = power(1)
        leave[0, rows, :lanes] = (vre * cre - vim * cim).astype(jnp.bfloat16)
        leave[0, rows, lanes:] = (-vre * cim - vim * cre).astype(jnp.bfloat16)
        xre, xim = power(2)
        inner_ref[rows, :lanes] = (xre * cre - xim * cim).astype(jnp.bfloat16)
        inner_ref[rows, lanes:] = (-xre * cim - xim * cre).astype(jnp.bfloat16)
    side = enter[0].shape[0]
    lane = lax.broadcasted_iota(jnp.int32, (side, 2 * lanes), 1) % lanes
    entering = enter[0]
    contract = (((1,), (1,)), ((), ()))
    zero = jnp.zeros_like(entering)
    ahead = lax.dot_general(
        jnp.where(lane < lanes // 2, entering, zero), inner_ref[...], contract,
        preferred_element_type=jnp.float32,
    )
    behind = lax.dot_general(
        jnp.where(lane < lanes // 2, zero, entering), inner_ref[...], contract,
        preferred_element_type=jnp.float32,
    )
    source = lax.broadcasted_iota(jnp.int32, (side, side), 0) // channels
    target = lax.broadcasted_iota(jnp.int32, (side, side), 1) // channels
    within[0] = (
        jnp.where(source <= target, ahead, 0.0) + jnp.where(source >= target, behind, 0.0)
    ).astype(jnp.bfloat16)


def make_tables(tables):
    own, channels, lanes = tables[0].shape
    side = BLOCK * channels
    whole = lambda value: pl.BlockSpec((1,) + value.shape[1:], lambda g: (g, 0, 0))
    out = lambda width: jax.ShapeDtypeStruct((own, side, width), jnp.bfloat16)
    outs = (out(side), out(2 * lanes), out(2 * lanes))
    return pl.pallas_call(
        table_kernel,
        grid=(own,),
        out_shape=outs,
        in_specs=[whole(value) for value in tables],
        out_specs=[whole(value) for value in outs],
        scratch_shapes=[pltpu.VMEM((side, 2 * lanes), jnp.bfloat16)],
        cost_estimate=pl.CostEstimate(
            flops=own * 4 * side * side * 2 * lanes * 4, bytes_accessed=own * side * side * 6, transcendentals=0
        ),
        name="tables",
    )(*tables)


def scan_kernel(length, u_ref, within, enter, leave, p_re, p_im, skip, out_ref):
    lanes = p_re.shape[2]
    rows = u_ref.shape[1]
    u = u_ref[0]
    local = jnp.dot(u, enter[0], preferred_element_type=jnp.float32)
    s_re, s_im = local[:, :lanes], local[:, lanes:]
    lane = lax.broadcasted_iota(jnp.int32, (rows, lanes), 1)
    place = lax.broadcasted_iota(jnp.int32, (rows, lanes), 0) % length
    forward = lane < lanes // 2

    def shifted(value, by):
        pad = jnp.zeros((by, lanes), jnp.float32)
        down = jnp.concatenate([pad, value[:-by]], axis=0)
        up = jnp.concatenate([value[by:], pad], axis=0)
        down = jnp.where(place >= by, down, 0.0)
        up = jnp.where(place < length - by, up, 0.0)
        return jnp.where(forward, down, up)

    hop = 1
    row = 3 * BLOCK
    while hop < length:
        h_re, h_im = p_re[0, row : row + 1, :], p_im[0, row : row + 1, :]
        m_re, m_im = shifted(s_re, hop), shifted(s_im, hop)
        s_re, s_im = s_re + h_re * m_re - h_im * m_im, s_im + h_re * m_im + h_im * m_re
        hop, row = 2 * hop, row + 1
    held = jnp.concatenate([shifted(s_re, 1), shifted(s_im, 1)], axis=1).astype(jnp.bfloat16)
    total = jnp.dot(u, within[0], preferred_element_type=jnp.float32)
    total += lax.dot_general(
        held, leave[0], (((1,), (1,)), ((), ())), preferred_element_type=jnp.float32
    )
    out_ref[0] = jax.nn.gelu(total + skip[0] * u.astype(jnp.float32)).astype(jnp.bfloat16)


def run_scan(blocks, within, enter, leave, p_re, p_im, skip, length):
    own, _, _ = blocks.shape
    whole = lambda value: pl.BlockSpec((1,) + value.shape[1:], lambda g: (g, 0, 0))
    operands = (blocks, within, enter, leave, p_re, p_im, skip)
    return pl.pallas_call(
        functools.partial(scan_kernel, length),
        grid=(own,),
        out_shape=jax.ShapeDtypeStruct(blocks.shape, jnp.bfloat16),
        in_specs=[whole(value) for value in operands],
        out_specs=whole(blocks),
        name="mixer",
    )(*operands)


def per_device(
    tokens,
    pre_gain,
    in_weight,
    decay_rate,
    frequency,
    log_step,
    input_matrix,
    output_matrix,
    skip_gain,
    glu_weight,
    up_weight,
    post_gain,
):
    seqs, local_len, _ = tokens.shape
    sp = lax.axis_size("sp")
    group_size = input_matrix.shape[-1] // decay_rate.shape[2]
    groups = decay_rate.shape[1]
    own = groups // sp
    near = local_len // BLOCK
    side = BLOCK * group_size
    length = near * sp
    offset = lax.axis_index("sp") * own

    dp = lax.axis_size("dp")
    packed = jnp.concatenate([glu_weight.T, up_weight.T], axis=0)
    glu_rows, packed_rows = glu_weight.shape[1], packed.shape[0]
    depth = packed.shape[1]
    packed = lax.all_gather(packed, "sp", axis=0, tiled=True)
    packed = lax.all_gather(packed, "dp", axis=0, tiled=True)
    packed = packed.reshape(dp, sp, packed_rows, depth)
    glu_full = packed[:, :, :glu_rows].reshape(dp, -1, depth)
    up_full = packed[:, :, glu_rows:].reshape(dp, -1, depth)
    in_full = relay_gather(in_weight.T, sp, dp)
    tables = own_tables(
        decay_rate, frequency, log_step, input_matrix, output_matrix, offset, own,
        max(1, (length - 1).bit_length()),
    )
    within, enter, leave = make_tables(tables)
    skip_rows = lax.dynamic_slice_in_dim(skip_gain.reshape(groups, 1, group_size), offset, own, 0)
    skip_rows = jnp.tile(skip_rows, (1, 1, BLOCK))
    normed = rms_scale(tokens, pre_gain).astype(jnp.bfloat16)
    mixer_in = jnp.einsum(
        "std,wd->stw", normed, in_full, preferred_element_type=jnp.float32
    ).astype(jnp.bfloat16)
    blocks = mixer_in.reshape(seqs, near, BLOCK, groups, group_size)
    blocks = jnp.transpose(blocks, (3, 0, 1, 2, 4)).reshape(groups, seqs, near, side)
    blocks = lax.all_to_all(blocks, "sp", split_axis=0, concat_axis=2, tiled=True)
    mixed = run_scan(
        blocks.reshape(own, seqs * length, side), within, enter, leave, tables[4], tables[5],
        skip_rows, length,
    )
    mixed = jnp.transpose(mixed.reshape(own, seqs, sp, near, side), (2, 0, 1, 3, 4))
    mixed = mixed.reshape(groups, seqs, near, side)
    mixed = lax.all_to_all(mixed, "sp", split_axis=0, concat_axis=0, tiled=True)
    mixed = mixed.reshape(groups, seqs, near, BLOCK, group_size)
    mixed = jnp.transpose(mixed, (1, 2, 3, 0, 4)).reshape(seqs, local_len, groups * group_size)

    def project(rows, weight):
        parts = [
            jnp.einsum(
                "stw,vw->stv", rows[..., k * depth : (k + 1) * depth], weight[k],
                preferred_element_type=jnp.float32,
            )
            for k in range(dp)
        ]
        return functools.reduce(jnp.add, parts)

    gate_pre = project(mixed, glu_full)
    gated = (mixed.astype(jnp.float32) * jax.nn.sigmoid(gate_pre)).astype(jnp.bfloat16)
    projected = project(gated, up_full)
    return rms_scale(projected, post_gain).astype(jnp.bfloat16)


def solution(mesh):
    return jax.shard_map(
        per_device,
        mesh=mesh,
        in_specs=(
            P("dp", "sp", None),
            P(),
            P("dp", "sp"),
            P(),
            P(),
            P(),
            P(),
            P(),
            P(),
            P("dp", "sp"),
            P("dp", "sp"),
            P(),
        ),
        out_specs=P("dp", "sp", None),
        check_vma=False,
    )
```

```python
import functools

import jax
import jax.numpy as jnp
from jax import lax
from jax.experimental import pallas as pl
from jax.experimental.pallas import tpu as pltpu
from jax.sharding import PartitionSpec as P


epsilon = 1e-06
BLOCK = 16


def rms_scale(values, gain):
    widened = values.astype(jnp.float32)
    return widened * lax.rsqrt(jnp.mean(widened * widened, axis=-1, keepdims=True) + epsilon) * gain


def own_tables(decay_rate, frequency, log_step, input_matrix, output_matrix, offset, own, hop_steps):
    take = functools.partial(lax.dynamic_slice_in_dim, start_index=offset, slice_size=own)
    rates = take(decay_rate, axis=1)
    frequencies = take(frequency, axis=1)
    delta = jnp.exp(take(log_step, axis=1))[..., None]
    damping = -rates * delta
    turning = frequencies * delta
    modulus = jnp.exp(damping)
    bar_im = modulus * jnp.sin(turning)
    half_sine = jnp.sin(0.5 * turning)
    minus_re = jnp.expm1(damping) * jnp.cos(turning) - 2.0 * half_sine * half_sine
    denominator = rates * rates + frequencies * frequencies
    factor_re = (bar_im * frequencies - minus_re * rates) / denominator
    factor_im = (-bar_im * rates - minus_re * frequencies) / denominator
    states = rates.shape[-1]
    matrix = take(input_matrix, axis=2).reshape(2, 2, own, states, -1)
    readout = take(output_matrix, axis=2).reshape(2, 2, own, -1, states)
    bbar_re = factor_re[..., None] * matrix[:, 0] - factor_im[..., None] * matrix[:, 1]
    bbar_im = factor_re[..., None] * matrix[:, 1] + factor_im[..., None] * matrix[:, 0]

    def lanes(value):
        return jnp.transpose(value, (1, 2, 0, 3)).reshape(own, value.shape[2], 2 * states)

    b_re = lanes(jnp.swapaxes(bbar_re, 2, 3))
    b_im = lanes(jnp.swapaxes(bbar_im, 2, 3))
    c_re = lanes(readout[:, 0])
    c_im = lanes(readout[:, 1])
    step = jnp.arange(BLOCK, dtype=jnp.float32)
    last = BLOCK - 1.0
    hops = BLOCK * 2.0 ** jnp.arange(hop_steps, dtype=jnp.float32)
    forward = jnp.concatenate([last - step, step + 1.0, step - last, hops])
    backward = jnp.concatenate([step, BLOCK - step, -step, hops])
    exponent = jnp.stack([forward, backward])[:, None, :, None]
    size = jnp.exp(damping[:, :, None, :] * exponent)
    angle = turning[:, :, None, :] * exponent
    return b_re, b_im, c_re, c_im, lanes(size * jnp.cos(angle)), lanes(size * jnp.sin(angle))


MESH = pl.DeviceIdType.MESH


def gather_kernel(sp, dp, shard, out, own_sem, send_sem, recv_sem, pass_sem, take_sem):
    rows, depth = shard.shape
    n_y, n_x = 2, 2
    n_z = sp // (n_y * n_x)
    me, core = lax.axis_index("sp"), lax.axis_index("dp")
    z, y, x = me // (n_y * n_x), (me // n_x) % n_y, me % n_x
    first = (rows // 2 + 15) // 16 * 16
    halves = ((0, first), (first, rows - first))

    def index(z_at, y_at, x_at):
        return (z_at * n_y + y_at) * n_x + x_at

    y_other, x_other = (y + 1) % n_y, (x + 1) % n_x
    y_peer, x_peer = index(z, y_other, x), index(z, y, x_other)
    z_peers = [index((z + hop) % n_z, y, x) for hop in range(1, n_z)]
    cores = [(core + hop) % dp for hop in range(1, dp)]
    barrier = pltpu.get_barrier_semaphore()
    for peer in [y_peer, x_peer] + z_peers:
        pl.semaphore_signal(barrier, inc=1, device_id={"sp": peer}, device_id_type=MESH)
    for peer in cores:
        pl.semaphore_signal(barrier, inc=1, device_id={"dp": peer}, device_id_type=MESH)
    pl.semaphore_wait(barrier, 2 + len(z_peers) + len(cores))

    sent, passed = [], []

    def place(who, half, column):
        start, size = halves[half]
        return out.at[
            pl.ds(pl.multiple_of(who * rows + start, 16), size),
            pl.ds(pl.multiple_of(column * depth, 128), depth),
        ]

    def source(who, half, mine):
        return shard.at[pl.ds(*halves[half]), :] if mine else place(who, half, core)

    def send(who, half, peer, mine=False):
        copy = pltpu.make_async_remote_copy(
            src_ref=source(who, half, mine),
            dst_ref=place(who, half, core),
            send_sem=send_sem.at[len(sent)],
            recv_sem=recv_sem.at[who, half],
            device_id={"sp": peer},
            device_id_type=MESH,
        )
        copy.start()
        sent.append(copy)

    def spread(who, half, mine=False):
        for hop, peer in enumerate(cores):
            copy = pltpu.make_async_remote_copy(
                src_ref=source(who, half, mine),
                dst_ref=place(who, half, core),
                send_sem=pass_sem.at[len(passed)],
                recv_sem=take_sem.at[hop, who, half],
                device_id={"dp": peer},
                device_id_type=MESH,
            )
            copy.start()
            passed.append(copy)

    def arrived(who, half):
        pltpu.make_async_remote_copy(
            src_ref=place(who, half, core),
            dst_ref=place(who, half, core),
            send_sem=send_sem.at[0],
            recv_sem=recv_sem.at[who, half],
            device_id={"sp": y_peer},
            device_id_type=MESH,
        ).wait_recv()

    own = [
        pltpu.make_async_copy(source(me, half, True), place(me, half, core), own_sem.at[half])
        for half in range(2)
    ]
    send(me, 0, y_peer, True)
    send(me, 1, x_peer, True)
    for peer in z_peers:
        send(me, 0, peer, True)
        send(me, 1, peer, True)
    send(me, 0, x_peer, True)
    send(me, 1, y_peer, True)
    for half in range(2):
        own[half].start()
        spread(me, half, True)
    for hop in range(n_z):
        at = (z + n_z - hop) % n_z
        if hop > 0:
            here = index(at, y, x)
            arrived(here, 0)
            send(here, 0, y_peer)
            arrived(here, 1)
            send(here, 1, x_peer)
            send(here, 0, x_peer)
            send(here, 1, y_peer)
            spread(here, 0)
            spread(here, 1)
        by_y, by_x = index(at, y_other, x), index(at, y, x_other)
        arrived(by_y, 0)
        send(by_y, 0, x_peer)
        spread(by_y, 0)
        arrived(by_x, 1)
        send(by_x, 1, y_peer)
        spread(by_x, 1)
    for hop in range(n_z):
        at = (z + n_z - hop) % n_z
        by_y, by_x = index(at, y_other, x), index(at, y, x_other)
        across = index(at, y_other, x_other)
        for who, half in ((by_x, 0), (by_y, 1), (across, 0), (across, 1)):
            arrived(who, half)
            spread(who, half)
    for hop in range(1, dp):
        column = (core + dp - hop) % dp
        for who in range(sp):
            for half in range(2):
                pltpu.make_async_remote_copy(
                    src_ref=place(who, half, column),
                    dst_ref=place(who, half, column),
                    send_sem=pass_sem.at[0],
                    recv_sem=take_sem.at[hop - 1, who, half],
                    device_id={"dp": cores[0]},
                    device_id_type=MESH,
                ).wait_recv()
    for copy in own:
        copy.wait()
    for copy in sent + passed:
        copy.wait_send()


def relay_gather(shard, sp, dp):
    rows, depth = shard.shape
    return pl.pallas_call(
        functools.partial(gather_kernel, sp, dp),
        out_shape=jax.ShapeDtypeStruct((sp * rows, dp * depth), shard.dtype),
        in_specs=[pl.BlockSpec(memory_space=pltpu.VMEM)],
        out_specs=pl.BlockSpec(memory_space=pl.ANY),
        scratch_shapes=[
            pltpu.SemaphoreType.DMA((2,)),
            pltpu.SemaphoreType.DMA((8 * sp,)),
            pltpu.SemaphoreType.DMA((sp, 2)),
            pltpu.SemaphoreType.DMA((2 * sp * (dp - 1),)),
            pltpu.SemaphoreType.DMA((dp - 1, sp, 2)),
        ],
        compiler_params=pltpu.CompilerParams(collective_id=1, has_side_effects=True),
        cost_estimate=pl.CostEstimate(flops=10**8, bytes_accessed=sp * rows * dp * depth * 2, transcendentals=0),
        name="relay_gather",
    )(shard)


def swap_kernel(dp, shard, out, send_sem, recv_sem):
    core = lax.axis_index("dp")
    barrier = pltpu.get_barrier_semaphore()
    for hop in range(1, dp):
        pl.semaphore_signal(barrier, inc=1, device_id={"dp": (core + hop) % dp}, device_id_type=MESH)
    pl.semaphore_wait(barrier, dp - 1)
    copies = [
        pltpu.make_async_remote_copy(
            src_ref=shard, dst_ref=out.at[hop - 1], send_sem=send_sem.at[hop - 1],
            recv_sem=recv_sem.at[hop - 1], device_id={"dp": (core + hop) % dp}, device_id_type=MESH,
        )
        for hop in range(1, dp)
    ]
    for copy in copies:
        copy.start()
    for copy in copies:
        copy.wait()


def swap(shard, dp):
    return pl.pallas_call(
        functools.partial(swap_kernel, dp),
        out_shape=jax.ShapeDtypeStruct((dp - 1,) + shard.shape, shard.dtype),
        in_specs=[pl.BlockSpec(memory_space=pl.ANY)],
        out_specs=pl.BlockSpec(memory_space=pl.ANY),
        scratch_shapes=[pltpu.SemaphoreType.DMA((dp - 1,)), pltpu.SemaphoreType.DMA((dp - 1,))],
        compiler_params=pltpu.CompilerParams(collective_id=2, has_side_effects=True),
        name="swap",
    )(shard)


def table_kernel(b_re, b_im, c_re, c_im, p_re, p_im, within, enter, leave, inner_ref):
    channels, lanes = b_re.shape[1:]
    bre, bim, cre, cim = b_re[0], b_im[0], c_re[0], c_im[0]
    for step in range(BLOCK):
        rows = pl.ds(step * channels, channels)

        def power(which):
            row = which * BLOCK + step
            return p_re[0, row : row + 1, :], p_im[0, row : row + 1, :]

        wre, wim = power(0)
        enter[0, rows, :lanes] = (wre * bre - wim * bim).astype(jnp.bfloat16)
        enter[0, rows, lanes:] = (wre * bim + wim * bre).astype(jnp.bfloat16)
        vre, vim = power(1)
        leave[0, rows, :lanes] = (vre * cre - vim * cim).astype(jnp.bfloat16)
        leave[0, rows, lanes:] = (-vre * cim - vim * cre).astype(jnp.bfloat16)
        xre, xim = power(2)
        inner_ref[rows, :lanes] = (xre * cre - xim * cim).astype(jnp.bfloat16)
        inner_ref[rows, lanes:] = (-xre * cim - xim * cre).astype(jnp.bfloat16)
    side = enter[0].shape[0]
    lane = lax.broadcasted_iota(jnp.int32, (side, 2 * lanes), 1) % lanes
    entering = enter[0]
    contract = (((1,), (1,)), ((), ()))
    zero = jnp.zeros_like(entering)
    ahead = lax.dot_general(
        jnp.where(lane < lanes // 2, entering, zero), inner_ref[...], contract,
        preferred_element_type=jnp.float32,
    )
    behind = lax.dot_general(
        jnp.where(lane < lanes // 2, zero, entering), inner_ref[...], contract,
        preferred_element_type=jnp.float32,
    )
    source = lax.broadcasted_iota(jnp.int32, (side, side), 0) // channels
    target = lax.broadcasted_iota(jnp.int32, (side, side), 1) // channels
    within[0] = (
        jnp.where(source <= target, ahead, 0.0) + jnp.where(source >= target, behind, 0.0)
    ).astype(jnp.bfloat16)


def make_tables(tables):
    own, channels, lanes = tables[0].shape
    side = BLOCK * channels
    whole = lambda value: pl.BlockSpec((1,) + value.shape[1:], lambda g: (g, 0, 0))
    out = lambda width: jax.ShapeDtypeStruct((own, side, width), jnp.bfloat16)
    outs = (out(side), out(2 * lanes), out(2 * lanes))
    return pl.pallas_call(
        table_kernel,
        grid=(own,),
        out_shape=outs,
        in_specs=[whole(value) for value in tables],
        out_specs=[whole(value) for value in outs],
        scratch_shapes=[pltpu.VMEM((side, 2 * lanes), jnp.bfloat16)],
        cost_estimate=pl.CostEstimate(
            flops=own * 4 * side * side * 2 * lanes * 4, bytes_accessed=own * side * side * 6, transcendentals=0
        ),
        name="tables",
    )(*tables)


def scan_kernel(length, u_ref, within, enter, leave, p_re, p_im, skip, out_ref):
    lanes = p_re.shape[2]
    rows = u_ref.shape[1]
    u = u_ref[0]
    local = jnp.dot(u, enter[0], preferred_element_type=jnp.float32)
    s_re, s_im = local[:, :lanes], local[:, lanes:]
    lane = lax.broadcasted_iota(jnp.int32, (rows, lanes), 1)
    place = lax.broadcasted_iota(jnp.int32, (rows, lanes), 0) % length
    forward = lane < lanes // 2

    def shifted(value, by):
        pad = jnp.zeros((by, lanes), jnp.float32)
        down = jnp.concatenate([pad, value[:-by]], axis=0)
        up = jnp.concatenate([value[by:], pad], axis=0)
        down = jnp.where(place >= by, down, 0.0)
        up = jnp.where(place < length - by, up, 0.0)
        return jnp.where(forward, down, up)

    hop = 1
    row = 3 * BLOCK
    while hop < length:
        h_re, h_im = p_re[0, row : row + 1, :], p_im[0, row : row + 1, :]
        m_re, m_im = shifted(s_re, hop), shifted(s_im, hop)
        s_re, s_im = s_re + h_re * m_re - h_im * m_im, s_im + h_re * m_im + h_im * m_re
        hop, row = 2 * hop, row + 1
    held = jnp.concatenate([shifted(s_re, 1), shifted(s_im, 1)], axis=1).astype(jnp.bfloat16)
    total = jnp.dot(u, within[0], preferred_element_type=jnp.float32)
    total += lax.dot_general(
        held, leave[0], (((1,), (1,)), ((), ())), preferred_element_type=jnp.float32
    )
    out_ref[0] = jax.nn.gelu(total + skip[0] * u.astype(jnp.float32)).astype(jnp.bfloat16)


def run_scan(blocks, within, enter, leave, p_re, p_im, skip, length):
    own, _, _ = blocks.shape
    whole = lambda value: pl.BlockSpec((1,) + value.shape[1:], lambda g: (g, 0, 0))
    operands = (blocks, within, enter, leave, p_re, p_im, skip)
    return pl.pallas_call(
        functools.partial(scan_kernel, length),
        grid=(own,),
        out_shape=jax.ShapeDtypeStruct(blocks.shape, jnp.bfloat16),
        in_specs=[whole(value) for value in operands],
        out_specs=whole(blocks),
        name="mixer",
    )(*operands)


def per_device(
    tokens,
    pre_gain,
    in_weight,
    decay_rate,
    frequency,
    log_step,
    input_matrix,
    output_matrix,
    skip_gain,
    glu_weight,
    up_weight,
    post_gain,
):
    seqs, local_len, _ = tokens.shape
    sp = lax.axis_size("sp")
    group_size = input_matrix.shape[-1] // decay_rate.shape[2]
    groups = decay_rate.shape[1]
    own = groups // sp
    near = local_len // BLOCK
    side = BLOCK * group_size
    length = near * sp
    offset = lax.axis_index("sp") * own

    dp = lax.axis_size("dp")
    packed = jnp.concatenate([glu_weight.T, up_weight.T], axis=0)
    glu_rows, packed_rows = glu_weight.shape[1], packed.shape[0]
    depth = packed.shape[1]
    packed = lax.all_gather(packed, "sp", axis=0, tiled=True)
    core = lax.axis_index("dp")
    others = swap(packed, dp)
    held = [packed] + [others[hop] for hop in range(dp - 1)]
    held = [value.reshape(sp, packed_rows, depth) for value in held]
    glu_full = [value[:, :glu_rows].reshape(-1, depth) for value in held]
    up_full = [value[:, glu_rows:].reshape(-1, depth) for value in held]
    in_full = relay_gather(in_weight.T, sp, dp)
    tables = own_tables(
        decay_rate, frequency, log_step, input_matrix, output_matrix, offset, own,
        max(1, (length - 1).bit_length()),
    )
    within, enter, leave = make_tables(tables)
    skip_rows = lax.dynamic_slice_in_dim(skip_gain.reshape(groups, 1, group_size), offset, own, 0)
    skip_rows = jnp.tile(skip_rows, (1, 1, BLOCK))
    normed = rms_scale(tokens, pre_gain).astype(jnp.bfloat16)
    mixer_in = jnp.einsum(
        "std,wd->stw", normed, in_full, preferred_element_type=jnp.float32
    ).astype(jnp.bfloat16)
    blocks = mixer_in.reshape(seqs, near, BLOCK, groups, group_size)
    blocks = jnp.transpose(blocks, (3, 0, 1, 2, 4)).reshape(groups, seqs, near, side)
    blocks = lax.all_to_all(blocks, "sp", split_axis=0, concat_axis=2, tiled=True)
    mixed = run_scan(
        blocks.reshape(own, seqs * length, side), within, enter, leave, tables[4], tables[5],
        skip_rows, length,
    )
    mixed = jnp.transpose(mixed.reshape(own, seqs, sp, near, side), (2, 0, 1, 3, 4))
    mixed = mixed.reshape(groups, seqs, near, side)
    mixed = lax.all_to_all(mixed, "sp", split_axis=0, concat_axis=0, tiled=True)
    mixed = mixed.reshape(groups, seqs, near, BLOCK, group_size)
    mixed = jnp.transpose(mixed, (1, 2, 3, 0, 4)).reshape(seqs, local_len, groups * group_size)

    def project(rows, weight):
        parts = [
            jnp.einsum(
                "stw,vw->stv", lax.dynamic_slice_in_dim(rows, (core + dp - k) % dp * depth, depth, 2), weight[k],
                preferred_element_type=jnp.float32,
            )
            for k in range(dp)
        ]
        return functools.reduce(jnp.add, parts)

    gate_pre = project(mixed, glu_full)
    gated = (mixed.astype(jnp.float32) * jax.nn.sigmoid(gate_pre)).astype(jnp.bfloat16)
    projected = project(gated, up_full)
    return rms_scale(projected, post_gain).astype(jnp.bfloat16)


def solution(mesh):
    return jax.shard_map(
        per_device,
        mesh=mesh,
        in_specs=(
            P("dp", "sp", None),
            P(),
            P("dp", "sp"),
            P(),
            P(),
            P(),
            P(),
            P(),
            P(),
            P("dp", "sp"),
            P("dp", "sp"),
            P(),
        ),
        out_specs=P("dp", "sp", None),
        check_vma=False,
    )
```
